32 devices in a mesh: rep: 4 (over z), fs: 2 (over y), tp: 4 (over x, core).
Axes of the slice: x: 2, y: 2, z: 4, core: 2. Of those that a mesh axis runs over, the one named last changes fastest.
Arguments:
- tokens: bfloat16 [1536, 2048], P('rep', ('fs', 'tp')), may hold values from -6 to 6
- cotangent: bfloat16 [1536, 2048], P('rep', ('fs', 'tp')), may hold values from -6 to 6
- gain: float32 [2048], replicated, may hold values from 0.1 to 1.9
- w_gate: bfloat16 [5376, 2048], P(('fs', 'tp')), may hold values from -0.125 to 0.125
- w_up: bfloat16 [5376, 2048], P(('fs', 'tp')), may hold values from -0.125 to 0.125
- w_down: bfloat16 [5376, 2048], P(('fs', 'tp')), may hold values from -0.078125 to 0.078125
Outputs:
- grad_input: bfloat16 [1536, 2048], P('rep', ('fs', 'tp'))
- grad_gain: float32 [2048], P(('fs', 'tp'))
- grad_gate: float32 [5376, 2048], P(('fs', 'tp'))
- grad_up: float32 [5376, 2048], P(('fs', 'tp'))
- grad_down: float32 [5376, 2048], P(('fs', 'tp'))
The draws below stay inside these ranges and needn't reach their ends.
All inputs are finite; a program needn't handle non-finite values.
Results may differ from the reference program's by a relative error of at most 0.006.
Values may be sent and summed in bfloat16 or wider, within the bound.
A program may use at most 128 MiB of HBM per device.

```python
import jax
import jax.numpy as jnp
from jax import lax

D = 2048
FF = 5376
TOKENS = 1536


def raised(array, key, source, target, parts, factor):
    def block_of(axis_at):
        return (jnp.arange(array.shape[axis_at]) // (array.shape[axis_at] // parts)).reshape((-1,) + (1,) * (array.ndim - 1 - axis_at))

    one_side = jax.random.permutation(key, parts)[block_of(target)]
    second = (block_of(target) + parts // 2) % parts
    return jnp.where((block_of(source) == one_side) | (block_of(source) == second), factor * array, array)


def block_scale(key, extent, pieces, least, top_value):
    loudness = 1.0
    for axis_at, parts in pieces:
        steps = jax.random.uniform(jax.random.fold_in(jax.random.fold_in(key, 6), axis_at), (parts,), jnp.float32, least / len(pieces), top_value / len(pieces))
        loudness = loudness * jnp.repeat(jnp.exp(steps), extent[axis_at] // parts).reshape((-1,) + (1,) * (len(extent) - 1 - axis_at))
    return loudness


def bell_draw(stream_key, dims, width, reach, pieces=(), held_as=jnp.bfloat16):
    level = block_scale(stream_key, dims, pieces, -0.22, 0.18) if pieces else 1.0
    values = jax.random.normal(stream_key, dims, jnp.float32) * width * level
    return jnp.minimum(jnp.maximum(values, -reach), reach).astype(held_as)


def noise_with(stream_key, dims, width, reach, pieces, heavy, kind=jnp.bfloat16):
    drawn = width * jax.random.normal(stream_key, dims, jnp.float32)
    if pieces:
        drawn = drawn * block_scale(stream_key, dims, pieces, -0.22, 0.18)
    return jnp.clip(raised(drawn, jax.random.fold_in(stream_key, 3), *heavy), -reach, reach).astype(kind)


def setup_inputs(seed: int = 0) -> dict:
    streams_of = jax.random.split(jax.random.key(seed), 7)
    tokens = bell_draw(streams_of[0], (TOKENS, D), 1.0, 6.0, ((0, 4), (1, 8)))
    cotangent = noise_with(streams_of[1], (TOKENS, D), 1.0, 6.0, ((0, 4), (1, 8)), (0, 1, 8, 2.0))
    gain = jnp.clip(1.0 + 0.18 * jax.random.normal(streams_of[2], (D,), jnp.float32), 0.1, 1.9)
    w_gate = bell_draw(streams_of[3], (FF, D), D ** -0.5, 0.125, ((0, 8),))
    w_up = bell_draw(streams_of[4], (FF, D), D ** -0.5, 0.125, ((0, 8),))
    w_down = bell_draw(streams_of[5], (FF, D), FF ** -0.5, 0.078125, ((0, 8),))
    return {"tokens": tokens, "cotangent": cotangent, "gain": gain, "w_gate": w_gate, "w_up": w_up, "w_down": w_down}


EPS = 1e-06

def reference(tokens, cotangent, gain, w_gate, w_up, w_down):
    xf = tokens.astype(jnp.float32)
    inv_rms = lax.rsqrt(lax.optimization_barrier(jnp.mean(xf * xf, axis=1, keepdims=True)) + EPS)
    unit = xf * inv_rms
    normed = (unit * gain).astype(jnp.bfloat16)
    gate = jnp.dot(normed, w_gate.T, preferred_element_type=jnp.float32)
    up = jnp.dot(normed, w_up.T, preferred_element_type=jnp.float32)
    sig = jax.nn.sigmoid(gate)
    active = gate * sig
    hidden = (active * up).astype(jnp.bfloat16)
    d_hidden = 0.5 * jnp.dot(cotangent, w_down.T, preferred_element_type=jnp.float32)
    d_gate = (d_hidden * up * sig * (1.0 + gate * (1.0 - sig))).astype(jnp.bfloat16)
    d_up = (d_hidden * active).astype(jnp.bfloat16)
    grad_down = 0.5 * jnp.dot(hidden.T, cotangent, preferred_element_type=jnp.float32)
    grad_gate = jnp.dot(d_gate.T, normed, preferred_element_type=jnp.float32)
    grad_up = jnp.dot(d_up.T, normed, preferred_element_type=jnp.float32)
    d_normed = jnp.dot(d_gate, w_gate, preferred_element_type=jnp.float32) + jnp.dot(d_up, w_up, preferred_element_type=jnp.float32)
    grad_gain = lax.optimization_barrier(jnp.sum(unit * d_normed, axis=0))
    d_unit = d_normed * gain
    row_mean = lax.optimization_barrier(jnp.mean(unit * d_unit, axis=1, keepdims=True))
    grad_input = (cotangent.astype(jnp.float32) + inv_rms * (d_unit - unit * row_mean)).astype(jnp.bfloat16)
    return (grad_input, grad_gain, grad_gate, grad_up, grad_down)
```

```python
import jax
import jax.numpy as jnp
from jax import lax
from jax.sharding import PartitionSpec as P

EPS = 1e-06
PLANE = ("fs", "tp")


def right_product(left, weight):
    return lax.dot_general(
        left, weight, (((1,), (1,)), ((), ())), preferred_element_type=jnp.float32
    )


def left_product(left, right):
    return lax.dot_general(
        left, right, (((0,), (0,)), ((), ())), preferred_element_type=jnp.float32
    )


def normalise(x, gain):
    xf = x.astype(jnp.float32)
    inv_rms = lax.rsqrt(jnp.mean(xf * xf, axis=1, keepdims=True) + EPS)
    return inv_rms, (xf * inv_rms * gain).astype(jnp.bfloat16)


def hidden_grads(normed, dy, w_gate, w_up, w_down):
    gate = right_product(normed, w_gate)
    up = right_product(normed, w_up)
    sig = jax.nn.sigmoid(gate)
    active = gate * sig
    hidden = (active * up).astype(jnp.bfloat16)
    d_hidden = 0.5 * right_product(dy, w_down)
    d_gate = (d_hidden * up * sig * (1.0 + gate * (1.0 - sig))).astype(jnp.bfloat16)
    d_up = (d_hidden * active).astype(jnp.bfloat16)
    return hidden, d_gate, d_up


def input_grads(tokens, cotangent, gain, inv_rms, d_gate, d_up, w_gate, w_up, wire):
    partial_value = jnp.dot(d_gate, w_gate, preferred_element_type=jnp.float32) + jnp.dot(
        d_up, w_up, preferred_element_type=jnp.float32
    )
    width = partial_value.shape[1]
    summed = lax.psum_scatter(
        partial_value.astype(wire), PLANE, scatter_dimension=1, tiled=True
    ).astype(jnp.float32)
    own_width = summed.shape[1]
    unit_own = tokens.astype(jnp.float32) * inv_rms
    gain_own = lax.dynamic_slice_in_dim(
        gain, lax.axis_index(PLANE) * own_width, own_width, 0
    )
    d_unit = summed * gain_own
    row_mean = lax.psum(jnp.sum(unit_own * d_unit, axis=1), PLANE) / width
    gain_part = jnp.sum(unit_own * summed, axis=0)
    grad_input = (
        cotangent.astype(jnp.float32) + inv_rms * (d_unit - unit_own * row_mean[:, None])
    ).astype(jnp.bfloat16)
    return grad_input, gain_part


def reduced(tokens, cotangent, gain, w_gate, w_up, w_down):
    full_x = lax.all_gather(tokens, PLANE, axis=1, tiled=True)
    full_dy = lax.all_gather(cotangent, PLANE, axis=1, tiled=True)
    inv_rms, normed = normalise(full_x, gain)
    hidden, d_gate, d_up = hidden_grads(normed, full_dy, w_gate, w_up, w_down)
    grad_down = 0.5 * left_product(hidden, full_dy)
    grad_gate = left_product(d_gate, normed)
    grad_up = left_product(d_up, normed)
    grad_input, gain_part = input_grads(
        tokens, cotangent, gain, inv_rms, d_gate, d_up, w_gate, w_up, jnp.float32
    )
    grad_gate, grad_up, grad_down, grad_gain = lax.psum(
        (grad_gate, grad_up, grad_down, gain_part), "rep"
    )
    return (grad_input, grad_gain, grad_gate, grad_up, grad_down)


def gathered(tokens, cotangent, gain, w_gate, w_up, w_down):
    rows, cols = tokens.shape
    both = lax.all_gather(jnp.stack([tokens, cotangent]), ("rep",) + PLANE)
    reps = lax.axis_size("rep")
    plane = lax.axis_size(PLANE)
    both = both.reshape(reps, plane, 2, rows, cols).transpose(2, 0, 3, 1, 4)
    both = both.reshape(2, reps * rows, plane * cols)
    inv_rms, normed = normalise(both[0], gain)
    dy = both[1]
    hidden, d_gate, d_up = hidden_grads(normed, dy, w_gate, w_up, w_down)
    start = lax.axis_index("rep") * rows
    own = lambda a: lax.dynamic_slice_in_dim(a, start, rows, 0)
    grad_input, gain_part = input_grads(
        tokens, cotangent, gain, own(inv_rms), own(d_gate), own(d_up), w_gate, w_up, jnp.bfloat16
    )
    grad_down = 0.5 * left_product(hidden, dy)
    grad_gate = left_product(d_gate, normed)
    grad_up = left_product(d_up, normed)
    return (grad_input, lax.psum(gain_part, "rep"), grad_gate, grad_up, grad_down)


def local(tokens, cotangent, gain, w_gate, w_up, w_down):
    reps = lax.axis_size("rep")
    token_bytes = 2 * 2 * tokens.shape[0] * reps * w_gate.shape[1]
    grad_bytes = 3 * 4 * w_gate.size
    plan = gathered if token_bytes < grad_bytes else reduced
    return plan(tokens, cotangent, gain, w_gate, w_up, w_down)


def solution(mesh):
    placed = (
        P("rep", PLANE),
        P("rep", PLANE),
        P(),
        P(PLANE, None),
        P(PLANE, None),
        P(PLANE, None),
    )
    return jax.shard_map(
        local,
        mesh=mesh,
        in_specs=placed,
        out_specs=(
            P("rep", PLANE),
            P(PLANE),
            P(PLANE, None),
            P(PLANE, None),
            P(PLANE, None),
        ),
        check_vma=False,
    )
```

```python
import functools

import jax
import jax.numpy as jnp
from jax import lax
from jax.experimental import pallas as pl
from jax.experimental.pallas import tpu as pltpu
from jax.sharding import PartitionSpec as P

EPS = 1e-06
PLANE = ("fs", "tp")


def right_product(left, weight):
    return lax.dot_general(
        left, weight, (((1,), (1,)), ((), ())), preferred_element_type=jnp.float32
    )


def left_product(left, right):
    return lax.dot_general(
        left, right, (((0,), (0,)), ((), ())), preferred_element_type=jnp.float32
    )


def normalise(x, gain):
    xf = x.astype(jnp.float32)
    inv_rms = lax.rsqrt(jnp.mean(xf * xf, axis=1, keepdims=True) + EPS)
    return inv_rms, (xf * inv_rms * gain).astype(jnp.bfloat16)


def hidden_grads(normed, dy, w_gate, w_up, w_down):
    gate = right_product(normed, w_gate)
    up = right_product(normed, w_up)
    sig = jax.nn.sigmoid(gate)
    active = gate * sig
    hidden = (active * up).astype(jnp.bfloat16)
    d_hidden = 0.5 * right_product(dy, w_down)
    d_gate = (d_hidden * up * sig * (1.0 + gate * (1.0 - sig))).astype(jnp.bfloat16)
    d_up = (d_hidden * active).astype(jnp.bfloat16)
    return hidden, d_gate, d_up


def hidden_sum(d_gate, d_up, w_gate, w_up):
    return jnp.dot(d_gate, w_gate, preferred_element_type=jnp.float32) + jnp.dot(
        d_up, w_up, preferred_element_type=jnp.float32
    )


def slotted_sums(rows_part, gain_part):
    rep, spot = lax.axis_index("rep"), lax.axis_index(PLANE)
    reps, plane = lax.axis_size("rep"), lax.axis_size(PLANE)
    rows, cols = rows_part.shape[0], gain_part.shape[0]
    slots = jnp.zeros((reps * rows + plane * cols,), jnp.float32)
    slots = lax.dynamic_update_slice(slots, rows_part, (rep * rows,))
    slots = lax.dynamic_update_slice(slots, gain_part, (reps * rows + spot * cols,))
    slots = lax.psum(slots, ("rep",) + PLANE)
    return (
        lax.dynamic_slice(slots, (rep * rows,), (rows,)),
        lax.dynamic_slice(slots, (reps * rows + spot * cols,), (cols,)),
    )


def input_grads(tokens, cotangent, gain, inv_rms, partial_value, sums):
    width = partial_value.shape[1]
    summed = lax.psum_scatter(
        partial_value, PLANE, scatter_dimension=1, tiled=True
    ).astype(jnp.float32)
    own_width = summed.shape[1]
    unit_own = tokens.astype(jnp.float32) * inv_rms
    gain_own = lax.dynamic_slice_in_dim(
        gain, lax.axis_index(PLANE) * own_width, own_width, 0
    )
    d_unit = summed * gain_own
    row_sum, gain_part = sums(jnp.sum(unit_own * d_unit, axis=1), jnp.sum(unit_own * summed, axis=0))
    row_mean = row_sum / width
    grad_input = (
        cotangent.astype(jnp.float32) + inv_rms * (d_unit - unit_own * row_mean[:, None])
    ).astype(jnp.bfloat16)
    return grad_input, gain_part


def reduced(tokens, cotangent, gain, w_gate, w_up, w_down):
    full_x = lax.all_gather(tokens, PLANE, axis=1, tiled=True)
    full_dy = lax.all_gather(cotangent, PLANE, axis=1, tiled=True)
    inv_rms, normed = normalise(full_x, gain)
    hidden, d_gate, d_up = hidden_grads(normed, full_dy, w_gate, w_up, w_down)
    grad_down = 0.5 * left_product(hidden, full_dy)
    grad_gate = left_product(d_gate, normed)
    grad_up = left_product(d_up, normed)
    grad_input, gain_part = input_grads(
        tokens, cotangent, gain, inv_rms, hidden_sum(d_gate, d_up, w_gate, w_up),
        lambda rows_part, gain_part: (lax.psum(rows_part, PLANE), gain_part),
    )
    grad_gate, grad_up, grad_down, grad_gain = lax.psum(
        (grad_gate, grad_up, grad_down, gain_part), "rep"
    )
    return (grad_input, grad_gain, grad_gate, grad_up, grad_down)


def gather_kernel(reps, tps, x_ref, dy_ref, out_ref, buf, send_sem, recv_sem, pair_sem, in_sem, out_sem):
    z, y, t = lax.axis_index("rep"), lax.axis_index("fs"), lax.axis_index("tp")
    rows, cols = x_ref.shape
    x_id = (z, y, lax.rem(t + 2, tps))
    y_id = (z, 1 - y, t)
    pair_id = (z, y, t + 1 - 2 * lax.rem(t, 2))
    up_id, down_id = (z + 1, y, t), (z - 1, y, t)
    has_up, has_down = z < reps - 1, z > 0
    column = (
        y * tps + t,
        y * tps + lax.rem(t + 2, tps),
        (1 - y) * tps + t,
        (1 - y) * tps + lax.rem(t + 2, tps),
    )
    pair_column = tuple(c + 1 - 2 * lax.rem(t, 2) for c in column)

    def piece(level, col, p):
        return buf.at[
            p,
            pl.ds(pl.multiple_of(level * rows, rows), rows),
            pl.ds(pl.multiple_of(col * cols, cols), cols),
        ]

    def copy(level, q, p, kind, target, landing):
        ref = piece(level, column[q], p)
        return pltpu.make_async_remote_copy(
            src_ref=ref, dst_ref=ref, send_sem=send_sem.at[kind, level, p], recv_sem=landing,
            device_id=target, device_id_type=pl.DeviceIdType.MESH,
        )

    def to_x(level, p):
        return copy(level, 0, p, 0, x_id, recv_sem.at[1, level, p])

    def to_y(level, p):
        return copy(level, 0, p, 1, y_id, recv_sem.at[2, level, p])

    def to_pair(level, q, p):
        return copy(level, q, p, 2 + q, pair_id, pair_sem.at[q, level, p])

    def to_up(level, p):
        return copy(level, 0, p, 6, up_id, recv_sem.at[0, level, p])

    def to_down(level, p):
        return copy(level, 0, p, 7, down_id, recv_sem.at[0, level, p])

    def corner(level, p):
        if p == 0:
            return copy(level, 1, p, 8, y_id, recv_sem.at[3, level, p])
        return copy(level, 2, p, 8, x_id, recv_sem.at[3, level, p])

    def landed(level, q, p):
        copy(level, q, p, 0, x_id, recv_sem.at[q, level, p]).wait_recv()

    loads = [
        pltpu.make_async_copy(ref, piece(z, column[0], p), in_sem.at[p])
        for p, ref in enumerate((x_ref, dy_ref))
    ]
    for load in loads:
        load.start()
    barrier = pltpu.get_barrier_semaphore()

    def greet(target):
        pl.semaphore_signal(barrier, inc=1, device_id=target, device_id_type=pl.DeviceIdType.MESH)

    for target in (x_id, y_id, pair_id):
        greet(target)
    pl.when(has_up)(lambda: greet(up_id))
    pl.when(has_down)(lambda: greet(down_id))
    along_z = lax.div(z + reps - 1, reps) + lax.div(2 * reps - 2 - z, reps)
    pl.semaphore_wait(barrier, 3 + along_z)

    for p in range(2):
        loads[p].wait()
        pl.when(has_up)(lambda p=p: to_up(z, p).start())
        pl.when(has_down)(lambda p=p: to_down(z, p).start())
        to_x(z, p).start()
        to_y(z, p).start()
        to_pair(z, 0, p).start()

    for far in range(1, reps):
        for p in range(2):

            @pl.when(z + far < reps)
            def _():
                level = z + far
                landed(level, 0, p)
                pl.when(has_down)(lambda: to_down(level, p).start())
                to_x(level, p).start()
                to_y(level, p).start()
                to_pair(level, 0, p).start()

            @pl.when(z - far >= 0)
            def _():
                level = z - far
                landed(level, 0, p)
                pl.when(has_up)(lambda: to_up(level, p).start())
                to_x(level, p).start()
                to_y(level, p).start()
                to_pair(level, 0, p).start()

    def each_level(act):
        act(z)
        for far in range(1, reps):
            pl.when(z + far < reps)(lambda far=far: act(z + far))
            pl.when(z - far >= 0)(lambda far=far: act(z - far))

    def relay(level):
        for q, p in ((1, 0), (2, 0), (1, 1), (2, 1)):
            landed(level, q, p)
            if q == p + 1:
                corner(level, p).start()
            to_pair(level, q, p).start()

    def corners(level):
        for p in range(2):
            landed(level, 3, p)
            to_pair(level, 3, p).start()

    def store(level, p):
        window = pl.ds(pl.multiple_of(level * rows, rows), rows)
        return pltpu.make_async_copy(
            buf.at[p, window], out_ref.at[p, window], out_sem.at[level, p]
        )

    def finish(level):
        for p in range(2):
            for q in range(4):
                ref = piece(level, pair_column[q], p)
                pltpu.make_async_remote_copy(
                    src_ref=ref, dst_ref=ref, send_sem=send_sem.at[2 + q, level, p],
                    recv_sem=pair_sem.at[q, level, p],
                    device_id=pair_id, device_id_type=pl.DeviceIdType.MESH,
                ).wait_recv()
            store(level, p).start()

    def drain(level):
        for p in range(2):
            to_x(level, p).wait_send()
            to_y(level, p).wait_send()
            corner(level, p).wait_send()
            for q in range(4):
                to_pair(level, q, p).wait_send()
            pl.when(jnp.logical_and(has_up, level <= z))(lambda p=p: to_up(level, p).wait_send())
            pl.when(jnp.logical_and(has_down, level >= z))(lambda p=p: to_down(level, p).wait_send())
            store(level, p).wait()

    for act in (relay, corners, finish, drain):
        each_level(act)


def gather_all(tokens, cotangent):
    reps, fss, tps = (lax.axis_size(name) for name in ("rep", "fs", "tp"))
    rows, cols = tokens.shape
    shape = (2, reps * rows, fss * tps * cols)
    return pl.pallas_call(
        functools.partial(gather_kernel, reps, tps),
        out_shape=jax.ShapeDtypeStruct(shape, tokens.dtype),
        in_specs=[pl.BlockSpec(memory_space=pl.ANY)] * 2,
        out_specs=pl.BlockSpec(memory_space=pl.ANY),
        scratch_shapes=[
            pltpu.VMEM(shape, tokens.dtype),
            pltpu.SemaphoreType.DMA((9, reps, 2)),
            pltpu.SemaphoreType.DMA((4, reps, 2)),
            pltpu.SemaphoreType.DMA((4, reps, 2)),
            pltpu.SemaphoreType.DMA((2,)),
            pltpu.SemaphoreType.DMA((reps, 2)),
        ],
        compiler_params=pltpu.CompilerParams(
            collective_id=0, has_side_effects=True, vmem_limit_bytes=48 * 2**20
        ),
    )(tokens, cotangent)


def gathered(tokens, cotangent, gain, w_gate, w_up, w_down):
    rows, cols = tokens.shape
    if (lax.axis_size("fs"), lax.axis_size("tp")) == (2, 4) and cols % 128 == 0:
        both = gather_all(tokens, cotangent)
    else:
        reps, plane = lax.axis_size("rep"), lax.axis_size(PLANE)
        both = lax.all_gather(jnp.stack([tokens, cotangent]), ("rep",) + PLANE)
        both = both.reshape(reps, plane, 2, rows, cols).transpose(2, 0, 3, 1, 4)
        both = both.reshape(2, reps * rows, plane * cols)
    inv_rms, normed = normalise(both[0], gain)
    dy = both[1]
    hidden, d_gate, d_up = hidden_grads(normed, dy, w_gate, w_up, w_down)
    start = lax.axis_index("rep") * rows
    own = lambda a: lax.dynamic_slice_in_dim(a, start, rows, 0)
    partial_value = hidden_sum(own(d_gate), own(d_up), w_gate, w_up).astype(jnp.bfloat16)
    partial_value, hidden, d_gate, d_up = lax.optimization_barrier(
        (partial_value, hidden, d_gate, d_up)
    )
    grad_input, grad_gain = input_grads(
        tokens, cotangent, gain, own(inv_rms), partial_value, slotted_sums
    )
    grad_down = 0.5 * left_product(hidden, dy)
    grad_gate = left_product(d_gate, normed)
    grad_up = left_product(d_up, normed)
    return (grad_input, grad_gain, grad_gate, grad_up, grad_down)


def local(tokens, cotangent, gain, w_gate, w_up, w_down):
    reps = lax.axis_size("rep")
    token_bytes = 2 * 2 * tokens.shape[0] * reps * w_gate.shape[1]
    grad_bytes = 3 * 4 * w_gate.size
    plan = gathered if token_bytes < grad_bytes else reduced
    return plan(tokens, cotangent, gain, w_gate, w_up, w_down)


def solution(mesh):
    placed = (
        P("rep", PLANE),
        P("rep", PLANE),
        P(),
        P(PLANE, None),
        P(PLANE, None),
        P(PLANE, None),
    )
    return jax.shard_map(
        local,
        mesh=mesh,
        in_specs=placed,
        out_specs=(
            P("rep", PLANE),
            P(PLANE),
            P(PLANE, None),
            P(PLANE, None),
            P(PLANE, None),
        ),
        check_vma=False,
    )
```
